32 devices in a mesh: sp: 4 (over z), fs: 4 (over y, x), tp: 2 (over core).
Axes of the slice: x: 2, y: 2, z: 4, core: 2. Of those that a mesh axis runs over, the one named last changes fastest.
Arguments:
- tokens: bfloat16 [4, 2048, 2048], P('fs', 'sp', 'tp'), may hold values from -6 to 6
- norm_gain: float32 [2048], replicated, may hold values from 0.1 to 1.9
- query_weight: bfloat16 [2048, 1024], P(('sp', 'fs'), 'tp'), may hold values from -0.125 to 0.125
- key_weight: bfloat16 [2048, 1024], P(('sp', 'fs'), 'tp'), may hold values from -0.125 to 0.125
- value_weight: bfloat16 [2048, 2048], P(('sp', 'fs'), 'tp'), may hold values from -0.125 to 0.125
- outgate_weight: bfloat16 [2048, 2048], P(('sp', 'fs'), 'tp'), may hold values from -0.125 to 0.125
- gate_weight: bfloat16 [2048, 2, 16], P(('sp', 'fs'), None, 'tp'), may hold values from -6 to 6
- forget_bias: float32 [16], P('tp')
- forget_shift: float32 [4, 16, 2048], P('fs', 'tp', 'sp'), may hold values from -1.5 to 0
- head_norm_gain: float32 [2048], P('tp'), may hold values from 0.1 to 1.9
- exit_weight: bfloat16 [2048, 2048], P(('sp', 'fs'), 'tp'), may hold values from -0.125 to 0.125
- entry_weight: bfloat16 [2048, 2048], P(('sp', 'fs'), 'tp'), may hold values from -0.125 to 0.125
- signal_weight: bfloat16 [2048, 2048], P(('sp', 'fs'), 'tp'), may hold values from -0.125 to 0.125
- conv_kernel: float32 [3, 2048], P(None, 'tp'), may hold values from -3.5 to 3.5
- merge_weight: bfloat16 [4096, 2048], P(('sp', 'fs'), 'tp'), may hold values from -0.09375 to 0.09375
Outputs:
- mixed: bfloat16 [4, 2048, 2048], P('fs', 'sp', 'tp')
The draws below stay inside these ranges and needn't reach their ends.
All inputs are finite; a program needn't handle non-finite values.
Results may differ from the reference program's by a relative error of at most 0.017.
The reference program's roundings to bfloat16 on the way count: a program that leaves them out, or rounds other values in their place, can miss the bound.
Values may be sent and summed in bfloat16 or wider, within the bound.
A program may use at most 128 MiB of HBM per device.

```python
import math
import jax
import jax.numpy as jnp
from jax import lax

D = 2048
HEADS = 16
DK = 64
DV = 128
CONV = 2048
BLOCK = 128
KERNEL = 3
TOK_DEV = 512
LEN = 2048
SEQS = 4


def draw_gate_weight(key, part):
    base = jax.random.normal(key, (D, 2, HEADS), jnp.float32) * D ** (-0.5)
    return jnp.clip(base, -6.0, 6.0).astype(jnp.bfloat16)


def draw_forget_bias(key, part):
    pick_key, quick_key, steady_key = jax.random.split(key, 3)
    share = 0.5
    fast = jax.random.uniform(pick_key, (HEADS,), jnp.float32) < share
    quick = jax.random.uniform(quick_key, (HEADS,), jnp.float32, 2.5, 4.0)
    constant_quantity = math.log(LEN) + jax.random.uniform(steady_key, (HEADS,), jnp.float32, 1.5, 2.5)
    return jnp.where(fast, quick, constant_quantity).astype(jnp.float32)


def draw_forget_shift(key, part):
    rate_key, place_key, depth_key = jax.random.split(key, 3)
    segments = LEN // TOK_DEV
    rates = jnp.exp(jax.random.uniform(rate_key, (SEQS, HEADS, segments), jnp.float32, math.log(0.05), 0.0)) / LEN
    constant_quantity = -jnp.repeat(rates, TOK_DEV, axis=2)
    places = jax.random.randint(place_key, (SEQS, HEADS, 2), 0, LEN)
    layer_tiers = jax.random.uniform(depth_key, (SEQS, HEADS, 2), jnp.float32, 0.22, 0.69)
    positions = jnp.arange(LEN, dtype=jnp.int32)
    agreement_tally = (positions[None, None, None, :] == places[..., None]).astype(jnp.float32)
    spike_clusters = -jnp.sum(agreement_tally * layer_tiers[..., None], axis=2)
    return (constant_quantity + spike_clusters).astype(jnp.float32)


def block_scale(rng, dims, shards, smallest, top_value):
    loudness, own = 1.0, jax.random.fold_in(rng, 6)
    for position, blocks in shards:
        steps = jnp.exp(jax.random.uniform(jax.random.fold_in(own, position), (blocks,), jnp.float32, smallest / len(shards), top_value / len(shards)))
        loudness = loudness * jnp.repeat(steps, dims[position] // blocks).reshape([-1 if axis == position else 1 for axis in range(len(dims))])
    return loudness


def centred(stream_key, dims, scale, limit, cuts=(), kind=jnp.bfloat16):
    result = scale * jax.random.normal(stream_key, dims, jnp.float32)
    if cuts:
        result = result * block_scale(stream_key, dims, cuts, -0.22, 0.18)
    return jnp.clip(result, -limit, limit).astype(kind)


def setup_inputs(seed: int = 0) -> dict:
    arg_keys = jax.random.split(jax.random.key(seed), 16)
    tokens = centred(arg_keys[0], (SEQS, LEN, D), 1.0, 6.0, ((0, 4), (1, 4), (2, 2)))
    norm_gain = jnp.clip(1.0 + 0.18 * jax.random.normal(arg_keys[1], (D,), jnp.float32), 0.1, 1.9)
    query_weight = centred(arg_keys[2], (D, HEADS * DK), D ** -0.5, 0.125, ((0, 16), (1, 2)))
    key_weight = centred(arg_keys[3], (D, HEADS * DK), D ** -0.5, 0.125, ((0, 16), (1, 2)))
    value_weight = centred(arg_keys[4], (D, HEADS * DV), D ** -0.5, 0.125, ((0, 16), (1, 2)))
    outgate_weight = centred(arg_keys[5], (D, HEADS * DV), D ** -0.5, 0.125, ((0, 16), (1, 2)))
    gate_weight = draw_gate_weight(jax.random.fold_in(arg_keys[15], 71), 0)
    forget_bias = draw_forget_bias(jax.random.fold_in(arg_keys[15], 71), 0)
    forget_shift = draw_forget_shift(jax.random.fold_in(arg_keys[15], 71), 0)
    head_norm_gain = jnp.clip(1.0 + 0.18 * jax.random.normal(arg_keys[9], (HEADS * DV,), jnp.float32), 0.1, 1.9)
    exit_weight = centred(arg_keys[10], (D, CONV), D ** -0.5, 0.125, ((0, 16), (1, 2)))
    entry_weight = centred(arg_keys[11], (D, CONV), D ** -0.5, 0.125, ((0, 16), (1, 2)))
    signal_weight = centred(arg_keys[12], (D, CONV), D ** -0.5, 0.125, ((0, 16), (1, 2)))
    conv_kernel = centred(arg_keys[13], (KERNEL, CONV), KERNEL ** -0.5, 3.5, ((1, 2),), jnp.float32)
    merge_weight = centred(arg_keys[14], (HEADS * DV + CONV, D), (HEADS * DV + CONV) ** -0.5, 0.09375, ((0, 16), (1, 2)))
    return {"tokens": tokens, "norm_gain": norm_gain, "query_weight": query_weight, "key_weight": key_weight, "value_weight": value_weight, "outgate_weight": outgate_weight, "gate_weight": gate_weight, "forget_bias": forget_bias, "forget_shift": forget_shift, "head_norm_gain": head_norm_gain, "exit_weight": exit_weight, "entry_weight": entry_weight, "signal_weight": signal_weight, "conv_kernel": conv_kernel, "merge_weight": merge_weight}


EPSILON = 1e-06
HIGHEST = lax.Precision.HIGHEST

def reference(tokens, norm_gain, query_weight, key_weight, value_weight, outgate_weight, gate_weight, forget_bias, forget_shift, head_norm_gain, exit_weight, entry_weight, signal_weight, conv_kernel, merge_weight):
    count = SEQS * LEN
    blocks = LEN // BLOCK
    flat = tokens.astype(jnp.float32)
    normed = (flat * lax.rsqrt(lax.optimization_barrier(jnp.mean(flat * flat, axis=-1, keepdims=True)) + EPSILON) * norm_gain).astype(jnp.bfloat16)
    rows = normed.reshape(count, D)

    def project(weight):
        return jnp.dot(rows, weight, preferred_element_type=jnp.float32)
    queries = project(query_weight).astype(jnp.bfloat16)
    keys = project(key_weight).astype(jnp.bfloat16)
    values = project(value_weight).astype(jnp.bfloat16)
    outgates = project(outgate_weight).astype(jnp.bfloat16)
    exit_rows = project(exit_weight).astype(jnp.bfloat16)
    entry_rows = project(entry_weight).astype(jnp.bfloat16)
    signal_rows = project(signal_weight).astype(jnp.bfloat16)
    gates = project(gate_weight.reshape(D, 2 * HEADS))

    def split_heads(array, width):
        return array.reshape(SEQS, blocks, BLOCK, HEADS, width).transpose(0, 3, 1, 2, 4).astype(jnp.float32)

    def lanes(array):
        return array.reshape(SEQS, blocks, BLOCK, HEADS).transpose(0, 3, 1, 2)
    inputs = lanes(gates[:, :HEADS])
    logs = lanes(jax.nn.log_sigmoid(gates[:, HEADS:] + forget_bias)) + forget_shift.reshape(SEQS, HEADS, blocks, BLOCK)
    query_float = split_heads(queries, DK)
    key_float = split_heads(keys, DK)
    value_float = split_heads(values, DV)
    scale = DK ** (-0.5)
    cumulative = jnp.cumsum(logs, axis=-1)
    last = cumulative[..., -1]
    weight_logs = last[..., None] - cumulative + inputs
    peak = lax.optimization_barrier(jnp.max(weight_logs, axis=-1))
    coefficient_array = jnp.exp(weight_logs - peak[..., None])
    scaled = key_float * scale
    states = jnp.einsum('bhcs,bhcsk,bhcsv->bhckv', coefficient_array, scaled, value_float, precision=HIGHEST)

    def step(carry, item):
        state, bounded_maximum = carry
        block_last, block_peak, block_state = item
        ceiling = jnp.maximum(block_last + bounded_maximum, block_peak)
        kept = jnp.exp(block_last + bounded_maximum - ceiling)
        added = jnp.exp(block_peak - ceiling)
        new_state = kept[..., None, None] * state + added[..., None, None] * block_state
        return ((new_state, ceiling), (state, bounded_maximum))
    start = (jnp.zeros((SEQS, HEADS, DK, DV), jnp.float32), jnp.zeros((SEQS, HEADS), jnp.float32))
    items = (jnp.moveaxis(last, 2, 0), jnp.moveaxis(peak, 2, 0), jnp.moveaxis(states, 2, 0))
    unused, before = lax.scan(step, start, items)
    state_prev = jnp.moveaxis(before[0], 0, 2)
    stable_prev = jnp.moveaxis(before[1], 0, 2)
    score_matrix = jnp.einsum('bhcjk,bhcsk->bhcjs', query_float, key_float) * scale
    causal = jnp.tril(jnp.ones((BLOCK, BLOCK), dtype=bool))
    decay = jnp.where(causal, cumulative[..., :, None] - cumulative[..., None, :] + inputs[..., None, :], -jnp.inf)
    inter = cumulative + stable_prev[..., None]
    ceiling = jnp.maximum(inter, lax.optimization_barrier(jnp.max(decay, axis=-1)))
    weighted = score_matrix * jnp.exp(decay - ceiling[..., None])
    rounded = lax.optimization_barrier(weighted.astype(jnp.bfloat16)).astype(jnp.float32)
    carried = jnp.exp(inter - ceiling)
    numerator = jnp.einsum('bhcjs,bhcsv->bhcjv', rounded, value_float)
    numerator = numerator + carried[..., None] * jnp.einsum('bhcjk,bhckv->bhcjv', query_float, state_prev, precision=HIGHEST)
    hidden = numerator * lax.rsqrt(lax.optimization_barrier(jnp.mean(numerator * numerator, axis=-1, keepdims=True)) + EPSILON)
    hidden = hidden.transpose(0, 2, 3, 1, 4).reshape(count, HEADS * DV) * head_norm_gain
    memory_out = (hidden * jax.nn.sigmoid(outgates.astype(jnp.float32))).astype(jnp.bfloat16)
    mixed_in = (entry_rows.astype(jnp.float32) * signal_rows.astype(jnp.float32)).astype(jnp.bfloat16)
    padded = jnp.pad(mixed_in.reshape(SEQS, LEN, CONV).astype(jnp.float32), ((0, 0), (KERNEL - 1, 0), (0, 0)))
    response = jnp.zeros((SEQS, LEN, CONV), jnp.float32)
    for tap in range(KERNEL):
        response = response + conv_kernel[tap] * padded[:, tap:tap + LEN]
    conv_out = (exit_rows.astype(jnp.float32) * response.reshape(count, CONV)).astype(jnp.bfloat16)
    concatenated_result = jnp.concatenate([memory_out, conv_out], axis=1)
    mixed = jnp.dot(concatenated_result, merge_weight, preferred_element_type=jnp.float32).astype(jnp.bfloat16)
    return mixed.reshape(SEQS, LEN, D)
```

```python
import jax
import jax.numpy as jnp
from jax import lax
from jax.sharding import PartitionSpec as P

DK = 64
DV = 128
BLOCK = 128
KERNEL = 3


EPSILON = 1e-06
EMPTY_LOG = -1e30
HIGHEST = lax.Precision.HIGHEST


def prefix(part, axis, combine, identity):
    place = lax.axis_index(axis)
    gathered = jax.tree.map(lambda a: lax.all_gather(a, axis), part)
    state = jax.tree.map(lambda a, e: jnp.zeros_like(a) + jnp.asarray(e, a.dtype), part, identity)

    def one(step, state):
        return combine(
            state, jax.tree.map(lambda a: lax.dynamic_index_in_dim(a, step, 0, False), gathered)
        )

    return lax.fori_loop(0, place, one, state)


def passed_along(value, axis, steps):
    count = lax.axis_size(axis)
    initial, last = (max(0, -steps), min(count, count - steps))
    return lax.ppermute(value, axis, [(source, source + steps) for source in range(initial, last)])


def combine(earlier, later):
    ceiling = jnp.maximum(later[2] + earlier[1], later[1])
    kept = jnp.exp(later[2] + earlier[1] - ceiling)
    added = jnp.exp(later[1] - ceiling)
    state = kept[..., None, None] * earlier[0] + added[..., None, None] * later[0]
    return (state, ceiling, earlier[2] + later[2])


def identity_state(heads):
    return (
        jnp.zeros((heads, DK, DV), jnp.float32),
        jnp.full((heads,), EMPTY_LOG, jnp.float32),
        jnp.zeros((heads,), jnp.float32),
    )


def add_product(left, piece):
    return jnp.dot(left, piece, preferred_element_type=jnp.float32)


def split_columns(total, stack):
    outputs = []
    offset = 0
    for weight in stack:
        outputs.append(total[:, offset : offset + weight.shape[1]])
        offset = offset + weight.shape[1]
    return outputs


def incoming_state(running):
    heads = running[1].shape[0]
    before = prefix((running[0], running[1], running[2]), "sp", combine, identity_state(heads))
    ceiling = jnp.maximum(before[1], before[2])
    shrink = jnp.exp(before[1] - ceiling)
    return (before[0] * shrink[:, None, None], ceiling, before[2])


def memory_states(keys, values, gates, forget_bias, forget_shift):
    count = gates.shape[0]
    heads = forget_bias.shape[0]
    blocks = count // BLOCK
    inputs = gates[:, :heads].reshape(blocks, BLOCK, heads)
    logs = jax.nn.log_sigmoid(gates[:, heads:] + forget_bias) + forget_shift[0].T
    cumulative = jnp.cumsum(logs.reshape(blocks, BLOCK, heads), axis=1)
    last = cumulative[:, -1]
    weight_logs = last[:, None, :] - cumulative + inputs
    peak = jnp.max(weight_logs, axis=1)
    coefficient_array = jnp.exp(weight_logs - peak[:, None, :])
    scaled = keys.reshape(blocks, BLOCK, heads, DK).astype(jnp.float32) * DK ** (-0.5)
    value_float = values.reshape(blocks, BLOCK, heads, DV).astype(jnp.float32)
    states = jnp.einsum(
        "csh,cshk,cshv->chkv", coefficient_array, scaled, value_float, precision=HIGHEST
    )
    running = identity_state(heads)
    prefixes = []
    for index in range(blocks):
        prefixes.append(running)
        running = combine(running, (states[index], peak[index], last[index]))
    leading_part = tuple((jnp.stack([item[member] for item in prefixes]) for member in range(3)))
    gate_apertures = combine(incoming_state(running), leading_part)
    return (gate_apertures, cumulative, inputs)


def memory_output(
    queries, keys, values, outgates, inputs, cumulative, gate_apertures, head_norm_gain
):
    blocks = cumulative.shape[0]
    heads = cumulative.shape[2]
    count = queries.shape[0]
    query_blocks = queries.reshape(blocks, BLOCK, heads, DK)
    key_blocks = keys.reshape(blocks, BLOCK, heads, DK)
    value_blocks = values.reshape(blocks, BLOCK, heads, DV)
    score_matrix = jnp.einsum(
        "cjhk,cshk->chjs", query_blocks, key_blocks, preferred_element_type=jnp.float32
    ) * DK ** (-0.5)
    cum_lanes = cumulative.transpose(0, 2, 1)
    input_lanes = inputs.transpose(0, 2, 1)
    causal = jnp.tril(jnp.ones((BLOCK, BLOCK), dtype=bool))
    decay = jnp.where(
        causal,
        cum_lanes[..., :, None] - cum_lanes[..., None, :] + input_lanes[..., None, :],
        -jnp.inf,
    )
    inter = cum_lanes + gate_apertures[1][..., None]
    ceiling = jnp.maximum(inter, jnp.max(decay, axis=-1))
    weighted = score_matrix * jnp.exp(decay - ceiling[..., None])
    numerator = jnp.einsum(
        "chjs,cshv->chjv",
        weighted.astype(jnp.bfloat16),
        value_blocks,
        preferred_element_type=jnp.float32,
    )
    query_float = query_blocks.astype(jnp.float32)
    carried = jnp.exp(inter - ceiling)
    numerator = numerator + carried[..., None] * jnp.einsum(
        "cjhk,chkv->chjv", query_float, gate_apertures[0], precision=HIGHEST
    )
    result = numerator * lax.rsqrt(
        jnp.mean(numerator * numerator, axis=-1, keepdims=True) + EPSILON
    )
    result = result.transpose(0, 2, 1, 3).reshape(count, heads * DV) * head_norm_gain
    return (result * jax.nn.sigmoid(outgates.astype(jnp.float32))).astype(jnp.bfloat16)


def local(
    tokens,
    norm_gain,
    query_weight,
    key_weight,
    value_weight,
    outgate_weight,
    gate_weight,
    forget_bias,
    forget_shift,
    head_norm_gain,
    exit_weight,
    entry_weight,
    signal_weight,
    conv_kernel,
    merge_weight,
):
    whole = lax.all_gather(tokens, "tp", axis=2, tiled=True)[0]
    count = whole.shape[0]
    flat = whole.astype(jnp.float32)
    normed = (
        flat * lax.rsqrt(jnp.mean(flat * flat, axis=-1, keepdims=True) + EPSILON) * norm_gain
    ).astype(jnp.bfloat16)
    gate_rows = gate_weight.reshape(gate_weight.shape[0], -1)
    state_stack = [key_weight, value_weight, gate_rows]
    other_stack = [query_weight, outgate_weight, exit_weight, entry_weight, signal_weight]
    stacked = jnp.concatenate(state_stack + other_stack, axis=1)
    total = add_product(normed, lax.all_gather(stacked, ("sp", "fs"), axis=0, tiled=True))
    columns = split_columns(total, state_stack + other_stack)
    keys = columns[0].astype(jnp.bfloat16)
    values = columns[1].astype(jnp.bfloat16)
    gate_apertures, cumulative, inputs = memory_states(
        keys, values, columns[2], forget_bias, forget_shift
    )
    others = columns[3:]
    queries = others[0].astype(jnp.bfloat16)
    outgates = others[1].astype(jnp.bfloat16)
    exit_rows = others[2].astype(jnp.bfloat16)
    entry_rows = others[3].astype(jnp.bfloat16)
    signal_rows = others[4].astype(jnp.bfloat16)
    mixed_in = (entry_rows.astype(jnp.float32) * signal_rows.astype(jnp.float32)).astype(
        jnp.bfloat16
    )
    rim = passed_along(mixed_in[count - (KERNEL - 1) :], "sp", 1)
    padded = jnp.concatenate([rim, mixed_in], axis=0).astype(jnp.float32)
    response = conv_kernel[0] * padded[0:count]
    for tap in range(1, KERNEL):
        response = response + conv_kernel[tap] * padded[tap : tap + count]
    conv_out = (exit_rows.astype(jnp.float32) * response).astype(jnp.bfloat16)
    memory_out = memory_output(
        queries, keys, values, outgates, inputs, cumulative, gate_apertures, head_norm_gain
    )
    memory_all, conv_all = (
        lax.all_gather(memory_out, "tp", axis=1, tiled=True),
        lax.all_gather(conv_out, "tp", axis=1, tiled=True),
    )
    concatenated_result = jnp.concatenate([memory_all, conv_all], axis=1)
    mixed = add_product(
        concatenated_result, lax.all_gather(merge_weight, ("sp", "fs"), axis=0, tiled=True)
    )
    return mixed.astype(jnp.bfloat16)[None]


def whole_states(keys, values, inputs, logs, blocks):
    heads = inputs.shape[1]
    inputs = inputs.reshape(blocks, BLOCK, heads)
    upto = jnp.tril(jnp.ones((BLOCK, BLOCK), jnp.float32))
    cumulative = jnp.einsum(
        "js,csh->cjh", upto, logs.reshape(blocks, BLOCK, heads), precision=HIGHEST
    )
    last = cumulative[:, -1]
    weight_logs = last[:, None, :] - cumulative + inputs
    peak = jnp.max(weight_logs, axis=1)
    coefficients = jnp.exp(weight_logs - peak[:, None, :])
    scaled = keys.reshape(blocks, BLOCK, heads, DK).astype(jnp.float32) * DK ** (-0.5)
    weighted_keys = scaled * coefficients[..., None]
    value_float = values.reshape(blocks, BLOCK, heads, DV).astype(jnp.float32)
    states = jnp.einsum("cshk,cshv->chkv", weighted_keys, value_float, precision=HIGHEST)
    place = jnp.arange(blocks)
    between = (place[None, :, None] < place[None, None, :]) & (
        place[None, None, :] < place[:, None, None]
    )
    decay = jnp.sum(jnp.where(between[..., None], last[None, None], 0.0), axis=2) + peak[None]
    earlier = (place[None, :] < place[:, None])[..., None]
    decay = jnp.where(earlier, decay, -jnp.inf)
    start = jnp.sum(jnp.where(earlier, last[None], 0.0), axis=1)
    ceiling = jnp.maximum(start, jnp.max(decay, axis=1))
    shares = jnp.exp(decay - ceiling[:, None])
    before = jnp.einsum("cdh,dhkv->chkv", shares, states, precision=HIGHEST)
    return ((before, ceiling), cumulative, inputs)


def resharded(
    tokens,
    norm_gain,
    query_weight,
    key_weight,
    value_weight,
    outgate_weight,
    gate_weight,
    forget_bias,
    forget_shift,
    head_norm_gain,
    exit_weight,
    entry_weight,
    signal_weight,
    conv_kernel,
    merge_weight,
):
    parts = lax.axis_size("sp")
    place = lax.axis_index("sp")
    depth = key_weight.shape[0]
    gates = gate_weight.shape[2]
    heads = gates // parts
    stack = [
        query_weight,
        key_weight,
        value_weight,
        outgate_weight,
        exit_weight,
        entry_weight,
        signal_weight,
        gate_weight.reshape(depth, 2, parts, heads).transpose(0, 2, 1, 3),
    ]
    stacked = jnp.concatenate([w.reshape(depth, parts, -1) for w in stack], axis=2)
    widths = [w.size // depth // parts for w in stack]
    sent = lax.all_to_all(stacked.transpose(1, 0, 2), "sp", 0, 0)
    rows = lax.all_gather(sent, "fs", axis=1)
    rows = rows.reshape(-1, rows.shape[-1])
    line = lax.all_gather(tokens[0], "sp", axis=0, tiled=True)
    whole = lax.all_gather(line, "tp", axis=1, tiled=True)
    count = whole.shape[0]
    flat = whole.astype(jnp.float32)
    normed = (
        flat * lax.rsqrt(jnp.mean(flat * flat, axis=-1, keepdims=True) + EPSILON) * norm_gain
    ).astype(jnp.bfloat16)
    total = add_product(normed, rows)
    columns = []
    offset = 0
    for width in widths:
        columns.append(total[:, offset : offset + width])
        offset = offset + width
    queries, keys, values, outgates, exit_rows, entry_rows, signal_rows = [
        c.astype(jnp.bfloat16) for c in columns[:7]
    ]
    gate_pre = columns[7]

    def own(array, axis, width):
        return lax.dynamic_slice_in_dim(array, place * width, width, axis)

    shift = lax.all_to_all(forget_shift[0].reshape(parts, heads, -1), "sp", 0, 0)
    shift = shift.transpose(1, 0, 2).reshape(heads, count)
    logs = jax.nn.log_sigmoid(gate_pre[:, heads:] + own(forget_bias, 0, heads)) + shift.T
    blocks = count // BLOCK
    apertures, cumulative, inputs = whole_states(keys, values, gate_pre[:, :heads], logs, blocks)
    channels = exit_rows.shape[1]
    taps = own(conv_kernel, 1, channels)
    mixed_in = (entry_rows.astype(jnp.float32) * signal_rows.astype(jnp.float32)).astype(
        jnp.bfloat16
    )
    padded = jnp.pad(mixed_in, ((KERNEL - 1, 0), (0, 0))).astype(jnp.float32)
    response = taps[0] * padded[0:count]
    for tap in range(1, KERNEL):
        response = response + taps[tap] * padded[tap : tap + count]
    conv_out = (exit_rows.astype(jnp.float32) * response).astype(jnp.bfloat16)
    memory_out = memory_output(
        queries,
        keys,
        values,
        outgates,
        inputs,
        cumulative,
        apertures,
        own(head_norm_gain, 0, heads * DV),
    )
    both = jnp.concatenate([memory_out, conv_out], axis=1)
    back = lax.all_to_all(both.reshape(parts, count // parts, -1), "sp", 0, 0)
    halves = lax.all_gather(back, "tp")
    memory_width = heads * DV
    memory_all = halves[..., :memory_width].transpose(2, 0, 1, 3).reshape(count // parts, -1)
    conv_all = halves[..., memory_width:].transpose(2, 0, 1, 3).reshape(count // parts, -1)
    merge = lax.all_gather(merge_weight, ("sp", "fs"), axis=0, tiled=True)
    mixed = add_product(jnp.concatenate([memory_all, conv_all], axis=1), merge)
    return mixed.astype(jnp.bfloat16)[None]


def solution(mesh):
    placed = (
        P("fs", "sp", "tp"),
        P(),
        P(("sp", "fs"), "tp"),
        P(("sp", "fs"), "tp"),
        P(("sp", "fs"), "tp"),
        P(("sp", "fs"), "tp"),
        P(("sp", "fs"), None, "tp"),
        P("tp"),
        P("fs", "tp", "sp"),
        P("tp"),
        P(("sp", "fs"), "tp"),
        P(("sp", "fs"), "tp"),
        P(("sp", "fs"), "tp"),
        P(None, "tp"),
        P(("sp", "fs"), "tp"),
    )
    sp, tp = mesh.shape["sp"], mesh.shape["tp"]

    def step(*args):
        heads, channels = args[6].shape[2], args[10].shape[1]
        even = heads % (sp * tp) == 0 and channels % (sp * tp * 128) == 0
        body = resharded if even else local
        return jax.shard_map(
            body, mesh=mesh, in_specs=placed, out_specs=P("fs", "sp", "tp"), check_vma=False
        )(*args)

    return step
```

```python
import jax
import jax.numpy as jnp
from jax import lax
from jax.experimental import pallas as pl
from jax.experimental.pallas import tpu as pltpu
from jax.sharding import PartitionSpec as P

DK = 64
DV = 128
BLOCK = 128
KERNEL = 3


EPSILON = 1e-06
EMPTY_LOG = -1e30
HIGHEST = lax.Precision.HIGHEST


def prefix(part, axis, combine, identity):
    place = lax.axis_index(axis)
    gathered = jax.tree.map(lambda a: lax.all_gather(a, axis), part)
    state = jax.tree.map(lambda a, e: jnp.zeros_like(a) + jnp.asarray(e, a.dtype), part, identity)

    def one(step, state):
        return combine(
            state, jax.tree.map(lambda a: lax.dynamic_index_in_dim(a, step, 0, False), gathered)
        )

    return lax.fori_loop(0, place, one, state)


def passed_along(value, axis, steps):
    count = lax.axis_size(axis)
    initial, last = (max(0, -steps), min(count, count - steps))
    return lax.ppermute(value, axis, [(source, source + steps) for source in range(initial, last)])


def combine(earlier, later):
    ceiling = jnp.maximum(later[2] + earlier[1], later[1])
    kept = jnp.exp(later[2] + earlier[1] - ceiling)
    added = jnp.exp(later[1] - ceiling)
    state = kept[..., None, None] * earlier[0] + added[..., None, None] * later[0]
    return (state, ceiling, earlier[2] + later[2])


def identity_state(heads):
    return (
        jnp.zeros((heads, DK, DV), jnp.float32),
        jnp.full((heads,), EMPTY_LOG, jnp.float32),
        jnp.zeros((heads,), jnp.float32),
    )


def add_product(left, piece):
    return jnp.dot(left, piece, preferred_element_type=jnp.float32)


def split_columns(total, stack):
    outputs = []
    offset = 0
    for weight in stack:
        outputs.append(total[:, offset : offset + weight.shape[1]])
        offset = offset + weight.shape[1]
    return outputs


def incoming_state(running):
    heads = running[1].shape[0]
    before = prefix((running[0], running[1], running[2]), "sp", combine, identity_state(heads))
    ceiling = jnp.maximum(before[1], before[2])
    shrink = jnp.exp(before[1] - ceiling)
    return (before[0] * shrink[:, None, None], ceiling, before[2])


def memory_states(keys, values, gates, forget_bias, forget_shift):
    count = gates.shape[0]
    heads = forget_bias.shape[0]
    blocks = count // BLOCK
    inputs = gates[:, :heads].reshape(blocks, BLOCK, heads)
    logs = jax.nn.log_sigmoid(gates[:, heads:] + forget_bias) + forget_shift[0].T
    cumulative = jnp.cumsum(logs.reshape(blocks, BLOCK, heads), axis=1)
    last = cumulative[:, -1]
    weight_logs = last[:, None, :] - cumulative + inputs
    peak = jnp.max(weight_logs, axis=1)
    coefficient_array = jnp.exp(weight_logs - peak[:, None, :])
    scaled = keys.reshape(blocks, BLOCK, heads, DK).astype(jnp.float32) * DK ** (-0.5)
    value_float = values.reshape(blocks, BLOCK, heads, DV).astype(jnp.float32)
    states = jnp.einsum(
        "csh,cshk,cshv->chkv", coefficient_array, scaled, value_float, precision=HIGHEST
    )
    running = identity_state(heads)
    prefixes = []
    for index in range(blocks):
        prefixes.append(running)
        running = combine(running, (states[index], peak[index], last[index]))
    leading_part = tuple((jnp.stack([item[member] for item in prefixes]) for member in range(3)))
    gate_apertures = combine(incoming_state(running), leading_part)
    return (gate_apertures, cumulative, inputs)


def memory_output(
    queries, keys, values, outgates, inputs, cumulative, gate_apertures, head_norm_gain
):
    blocks = cumulative.shape[0]
    heads = cumulative.shape[2]
    count = queries.shape[0]
    query_blocks = queries.reshape(blocks, BLOCK, heads, DK)
    key_blocks = keys.reshape(blocks, BLOCK, heads, DK)
    value_blocks = values.reshape(blocks, BLOCK, heads, DV)
    score_matrix = jnp.einsum(
        "cjhk,cshk->chjs", query_blocks, key_blocks, preferred_element_type=jnp.float32
    ) * DK ** (-0.5)
    cum_lanes = cumulative.transpose(0, 2, 1)
    input_lanes = inputs.transpose(0, 2, 1)
    causal = jnp.tril(jnp.ones((BLOCK, BLOCK), dtype=bool))
    decay = jnp.where(
        causal,
        cum_lanes[..., :, None] - cum_lanes[..., None, :] + input_lanes[..., None, :],
        -jnp.inf,
    )
    inter = cum_lanes + gate_apertures[1][..., None]
    ceiling = jnp.maximum(inter, jnp.max(decay, axis=-1))
    weighted = score_matrix * jnp.exp(decay - ceiling[..., None])
    numerator = jnp.einsum(
        "chjs,cshv->chjv",
        weighted.astype(jnp.bfloat16),
        value_blocks,
        preferred_element_type=jnp.float32,
    )
    query_float = query_blocks.astype(jnp.float32)
    carried = jnp.exp(inter - ceiling)
    numerator = numerator + carried[..., None] * jnp.einsum(
        "cjhk,chkv->chjv", query_float, gate_apertures[0], precision=HIGHEST
    )
    result = numerator * lax.rsqrt(
        jnp.mean(numerator * numerator, axis=-1, keepdims=True) + EPSILON
    )
    result = result.transpose(0, 2, 1, 3).reshape(count, heads * DV) * head_norm_gain
    return (result * jax.nn.sigmoid(outgates.astype(jnp.float32))).astype(jnp.bfloat16)


def local(
    tokens,
    norm_gain,
    query_weight,
    key_weight,
    value_weight,
    outgate_weight,
    gate_weight,
    forget_bias,
    forget_shift,
    head_norm_gain,
    exit_weight,
    entry_weight,
    signal_weight,
    conv_kernel,
    merge_weight,
):
    whole = lax.all_gather(tokens, "tp", axis=2, tiled=True)[0]
    count = whole.shape[0]
    flat = whole.astype(jnp.float32)
    normed = (
        flat * lax.rsqrt(jnp.mean(flat * flat, axis=-1, keepdims=True) + EPSILON) * norm_gain
    ).astype(jnp.bfloat16)
    gate_rows = gate_weight.reshape(gate_weight.shape[0], -1)
    state_stack = [key_weight, value_weight, gate_rows]
    other_stack = [query_weight, outgate_weight, exit_weight, entry_weight, signal_weight]
    stacked = jnp.concatenate(state_stack + other_stack, axis=1)
    total = add_product(normed, lax.all_gather(stacked, ("sp", "fs"), axis=0, tiled=True))
    columns = split_columns(total, state_stack + other_stack)
    keys = columns[0].astype(jnp.bfloat16)
    values = columns[1].astype(jnp.bfloat16)
    gate_apertures, cumulative, inputs = memory_states(
        keys, values, columns[2], forget_bias, forget_shift
    )
    others = columns[3:]
    queries = others[0].astype(jnp.bfloat16)
    outgates = others[1].astype(jnp.bfloat16)
    exit_rows = others[2].astype(jnp.bfloat16)
    entry_rows = others[3].astype(jnp.bfloat16)
    signal_rows = others[4].astype(jnp.bfloat16)
    mixed_in = (entry_rows.astype(jnp.float32) * signal_rows.astype(jnp.float32)).astype(
        jnp.bfloat16
    )
    rim = passed_along(mixed_in[count - (KERNEL - 1) :], "sp", 1)
    padded = jnp.concatenate([rim, mixed_in], axis=0).astype(jnp.float32)
    response = conv_kernel[0] * padded[0:count]
    for tap in range(1, KERNEL):
        response = response + conv_kernel[tap] * padded[tap : tap + count]
    conv_out = (exit_rows.astype(jnp.float32) * response).astype(jnp.bfloat16)
    memory_out = memory_output(
        queries, keys, values, outgates, inputs, cumulative, gate_apertures, head_norm_gain
    )
    memory_all, conv_all = (
        lax.all_gather(memory_out, "tp", axis=1, tiled=True),
        lax.all_gather(conv_out, "tp", axis=1, tiled=True),
    )
    concatenated_result = jnp.concatenate([memory_all, conv_all], axis=1)
    mixed = add_product(
        concatenated_result, lax.all_gather(merge_weight, ("sp", "fs"), axis=0, tiled=True)
    )
    return mixed.astype(jnp.bfloat16)[None]


def whole_states(keys, values, inputs, logs, blocks):
    heads = inputs.shape[1]
    inputs = inputs.reshape(blocks, BLOCK, heads)
    upto = jnp.tril(jnp.ones((BLOCK, BLOCK), jnp.float32))
    cumulative = jnp.einsum(
        "js,csh->cjh", upto, logs.reshape(blocks, BLOCK, heads), precision=HIGHEST
    )
    last = cumulative[:, -1]
    weight_logs = last[:, None, :] - cumulative + inputs
    peak = jnp.max(weight_logs, axis=1)
    coefficients = jnp.exp(weight_logs - peak[:, None, :])
    scaled = keys.reshape(blocks, BLOCK, heads, DK).astype(jnp.float32) * DK ** (-0.5)
    weighted_keys = scaled * coefficients[..., None]
    value_float = values.reshape(blocks, BLOCK, heads, DV).astype(jnp.float32)
    states = jnp.einsum("cshk,cshv->chkv", weighted_keys, value_float, precision=HIGHEST)
    place = jnp.arange(blocks)
    between = (place[None, :, None] < place[None, None, :]) & (
        place[None, None, :] < place[:, None, None]
    )
    decay = jnp.sum(jnp.where(between[..., None], last[None, None], 0.0), axis=2) + peak[None]
    earlier = (place[None, :] < place[:, None])[..., None]
    decay = jnp.where(earlier, decay, -jnp.inf)
    start = jnp.sum(jnp.where(earlier, last[None], 0.0), axis=1)
    ceiling = jnp.maximum(start, jnp.max(decay, axis=1))
    shares = jnp.exp(decay - ceiling[:, None])
    before = jnp.einsum("cdh,dhkv->chkv", shares, states, precision=HIGHEST)
    return ((before, ceiling), cumulative, inputs)


def spread_kernel(first, second, n, m, x_ref, out_ref, local_sem, send, recv, send_on, recv_on):
    me = lax.axis_index(first)
    mine = lax.axis_index(second)
    barrier = pltpu.get_barrier_semaphore()
    mesh_ids = pl.DeviceIdType.MESH
    for k in range(1, n):
        pl.semaphore_signal(
            barrier, inc=1, device_id={first: lax.rem(me + k, n)}, device_id_type=mesh_ids
        )
    for k in range(1, m):
        pl.semaphore_signal(
            barrier, inc=1, device_id={second: lax.rem(mine + k, m)}, device_id_type=mesh_ids
        )
    pl.semaphore_wait(barrier, n + m - 2)
    copies = []
    for k in range(1, n):
        peer = lax.rem(me + k, n)
        copy = pltpu.make_async_remote_copy(
            src_ref=x_ref.at[peer],
            dst_ref=out_ref.at[me, mine],
            send_sem=send.at[k - 1],
            recv_sem=recv.at[k - 1],
            device_id={first: peer},
            device_id_type=mesh_ids,
        )
        copy.start()
        copies.append(copy)
    kept = pltpu.make_async_copy(x_ref.at[me], out_ref.at[me, mine], local_sem)
    kept.start()
    onward = []
    for k in range(n):
        source = lax.rem(me - k + n, n)
        if k > 0:
            copies[k - 1].wait_recv()
        block = x_ref.at[me] if k == 0 else out_ref.at[source, mine]
        for j in range(1, m):
            copy = pltpu.make_async_remote_copy(
                src_ref=block,
                dst_ref=out_ref.at[source, mine],
                send_sem=send_on.at[k, j - 1],
                recv_sem=recv_on.at[k, j - 1],
                device_id={second: lax.rem(mine + j, m)},
                device_id_type=mesh_ids,
            )
            copy.start()
            onward.append(copy)
    kept.wait()
    for copy in copies:
        copy.wait_send()
    for k in range(n):
        for j in range(1, m):
            copy = onward[k * (m - 1) + j - 1]
            copy.wait_send()
            copy.wait_recv()


def spread(x, first, second, number):
    n, m = lax.axis_size(first), lax.axis_size(second)
    shape = (n, m) + x.shape[1:]
    size = x.size * x.dtype.itemsize * m
    return pl.pallas_call(
        lambda *refs: spread_kernel(first, second, n, m, *refs),
        out_shape=jax.ShapeDtypeStruct(shape, x.dtype),
        in_specs=[pl.BlockSpec(memory_space=pltpu.VMEM)],
        out_specs=pl.BlockSpec(memory_space=pltpu.VMEM),
        scratch_shapes=[
            pltpu.SemaphoreType.DMA,
            pltpu.SemaphoreType.DMA((n - 1,)),
            pltpu.SemaphoreType.DMA((n - 1,)),
            pltpu.SemaphoreType.DMA((n, m - 1)),
            pltpu.SemaphoreType.DMA((n, m - 1)),
        ],
        compiler_params=pltpu.CompilerParams(collective_id=number, has_side_effects=True),
        cost_estimate=pl.CostEstimate(flops=0, bytes_accessed=30 * size, transcendentals=0),
    )(x)


def both_halves(own, axis):
    if lax.axis_size("tp") != 2:
        return lax.all_gather(own, "tp", axis=axis, tiled=True)
    other = lax.ppermute(own, "tp", [(0, 1), (1, 0)])
    first = lax.axis_index("tp") == 0
    return jnp.concatenate(
        [jnp.where(first, own, other), jnp.where(first, other, own)], axis=axis
    )


def resharded(
    tokens,
    norm_gain,
    query_weight,
    key_weight,
    value_weight,
    outgate_weight,
    gate_weight,
    forget_bias,
    forget_shift,
    head_norm_gain,
    exit_weight,
    entry_weight,
    signal_weight,
    conv_kernel,
    merge_weight,
):
    parts = lax.axis_size("sp")
    place = lax.axis_index("sp")
    depth = key_weight.shape[0]
    gates = gate_weight.shape[2]
    heads = gates // parts
    stack = [
        query_weight,
        key_weight,
        value_weight,
        outgate_weight,
        exit_weight,
        entry_weight,
        signal_weight,
        gate_weight.reshape(depth, 2, parts, heads).swapaxes(1, 2).reshape(depth, -1),
    ]
    widths = [w.size // depth // parts for w in stack]
    spare = jnp.zeros((depth, -sum(widths) % 128), jnp.bfloat16)
    stacked = jnp.stack(
        [
            jnp.concatenate(
                [w[:, p * width : (p + 1) * width] for w, width in zip(stack, widths)] + [spare],
                axis=1,
            )
            for p in range(parts)
        ]
    )
    rows = spread(stacked, "sp", "fs", 0)
    rows = rows.reshape(-1, rows.shape[-1])
    line = lax.all_gather(tokens[0], "sp", axis=0, tiled=True)
    rows, line, merge_weight = lax.optimization_barrier((rows, line, merge_weight))
    whole = both_halves(line, 1)
    count = whole.shape[0]
    flat = whole.astype(jnp.float32)
    normed = (
        flat * lax.rsqrt(jnp.mean(flat * flat, axis=-1, keepdims=True) + EPSILON) * norm_gain
    ).astype(jnp.bfloat16)
    total = add_product(normed, rows)
    columns = []
    offset = 0
    for width in widths:
        columns.append(total[:, offset : offset + width])
        offset = offset + width
    queries, keys, values, outgates, exit_rows, entry_rows, signal_rows = [
        c.astype(jnp.bfloat16) for c in columns[:7]
    ]
    gate_pre = columns[7]

    def own(array, axis, width):
        return lax.dynamic_slice_in_dim(array, place * width, width, axis)

    shift = lax.all_to_all(forget_shift[0].reshape(parts, heads, -1), "sp", 0, 0)
    shift = shift.transpose(1, 0, 2).reshape(heads, count)
    logs = jax.nn.log_sigmoid(gate_pre[:, heads:] + own(forget_bias, 0, heads)) + shift.T
    blocks = count // BLOCK
    apertures, cumulative, inputs = whole_states(keys, values, gate_pre[:, :heads], logs, blocks)
    channels = exit_rows.shape[1]
    taps = own(conv_kernel, 1, channels)
    mixed_in = (entry_rows.astype(jnp.float32) * signal_rows.astype(jnp.float32)).astype(
        jnp.bfloat16
    )
    padded = jnp.pad(mixed_in, ((KERNEL - 1, 0), (0, 0))).astype(jnp.float32)
    response = taps[0] * padded[0:count]
    for tap in range(1, KERNEL):
        response = response + taps[tap] * padded[tap : tap + count]
    conv_out = (exit_rows.astype(jnp.float32) * response).astype(jnp.bfloat16)
    memory_out = memory_output(
        queries,
        keys,
        values,
        outgates,
        inputs,
        cumulative,
        apertures,
        own(head_norm_gain, 0, heads * DV),
    )
    both = jnp.concatenate([memory_out, conv_out], axis=1)
    halves = spread(both.reshape(parts, count // parts, -1), "sp", "tp", 1)
    memory_width = heads * DV
    pieces = [(t, p) for t in range(halves.shape[1]) for p in range(parts)]
    merged_in = jnp.concatenate(
        [halves[p, t, :, :memory_width] for t, p in pieces]
        + [halves[p, t, :, memory_width:] for t, p in pieces],
        axis=1,
    )
    merge = lax.all_gather(merge_weight, ("sp", "fs"), axis=0, tiled=True)
    mixed = add_product(merged_in, merge)
    return mixed.astype(jnp.bfloat16)[None]


def solution(mesh):
    placed = (
        P("fs", "sp", "tp"),
        P(),
        P(("sp", "fs"), "tp"),
        P(("sp", "fs"), "tp"),
        P(("sp", "fs"), "tp"),
        P(("sp", "fs"), "tp"),
        P(("sp", "fs"), None, "tp"),
        P("tp"),
        P("fs", "tp", "sp"),
        P("tp"),
        P(("sp", "fs"), "tp"),
        P(("sp", "fs"), "tp"),
        P(("sp", "fs"), "tp"),
        P(None, "tp"),
        P(("sp", "fs"), "tp"),
    )
    sp, tp = mesh.shape["sp"], mesh.shape["tp"]

    def step(*args):
        heads, channels = args[6].shape[2], args[10].shape[1]
        many = min(sp, mesh.shape["fs"], tp) > 1
        even = heads % (sp * tp) == 0 and channels % (sp * tp * 128) == 0
        body = resharded if many and even else local
        return jax.shard_map(
            body, mesh=mesh, in_specs=placed, out_specs=P("fs", "sp", "tp"), check_vma=False
        )(*args)

    return step
```
